512 devices in a mesh: kv: 128 (over z, y, core), tp: 4 (over x).
Axes of the slice: x: 4, y: 8, z: 8, core: 2. Of those that a mesh axis runs over, the one named last changes fastest.
Arguments:
- piece_tokens: bfloat16 [512, 2048], P('kv'), may hold values from -6 to 6
- decode_tokens: bfloat16 [128, 2048], P('kv'), may hold values from -6 to 6
- prompt_fill: int32 [1], replicated, may hold values from 16384 to 32256
- decode_fill: int32 [128], P('kv'), may hold values from 1 to 767, 49152 in all
- prompt_cache: bfloat16 [32768, 544], P('kv'), may hold values from -600 to 600
- decode_cache: bfloat16 [128, 768, 544], P('kv'), may hold values from -600 to 600
- input_gain: float32 [2048], replicated, may hold values from 0.1 to 1.9
- query_gain: float32 [768], replicated, may hold values from 0.1 to 1.9
- latent_gain: float32 [512], replicated, may hold values from 0.1 to 1.9
- query_down: bfloat16 [2048, 768], P(None, 'tp'), may hold values from -0.125 to 0.125
- latent_down: bfloat16 [2048, 512], P(None, 'tp'), may hold values from -0.125 to 0.125
- rope_down: bfloat16 [2048, 32], replicated, may hold values from -0.125 to 0.125
- query_up: bfloat16 [768, 1024], P(None, 'tp'), may hold values from -0.21875 to 0.21875
- qrope_up: bfloat16 [768, 512], P(None, 'tp'), may hold values from -0.21875 to 0.21875
- key_up: bfloat16 [16, 64, 512], P('tp'), may hold values from -0.25 to 0.25
- value_up: bfloat16 [16, 512, 64], P('tp'), may hold values from -4 to 4
- out_proj: bfloat16 [1024, 2048], P('tp'), may hold values from -4 to 4
Outputs:
- piece_out: bfloat16 [512, 2048], P('kv')
- decode_out: bfloat16 [128, 2048], P('kv')
- piece_rows: bfloat16 [512, 544], P('kv')
- decode_rows: bfloat16 [128, 544], P('kv')
The draws below stay inside these ranges and needn't reach their ends.
Inputs may be any that keep to these rules, and one draw needn't show every extreme that they name: `prompt_fill`: the piece takes the 512 positions that follow the cache's filled positions. `decode_fill`: a decoding sequence's new token takes the position that follows its filled ones.
All inputs are finite; a program needn't handle non-finite values. No bound on the sum of `decode_fill` on one device may be relied on, other than what follows from the above.
Results may differ from the reference program's by a relative error of at most 0.035.
Values may be sent and summed in bfloat16 or wider, within the bound.
A program may use at most 64 MiB of HBM per device.

```python
import math
import jax
import jax.numpy as jnp
import numpy as np
from jax import lax

D = 2048
H = 16
QL = 768
KL = 512
NOPE = 64
ROPE = 32
VD = 64
CACHE_DEV = 256
DEC_LEN = 768
PIECE = 512
CACHE = 32768
DEC = 128
N_KV = 128
N_TP = 4


def draw_prompt_cache(key, part):
    values = jnp.clip(jax.random.normal(key, (CACHE, KL + ROPE), jnp.float32), -5.0, 5.0)
    return values.astype(jnp.bfloat16)


def draw_decode_cache(key, part):
    values = jnp.clip(jax.random.normal(key, (DEC, DEC_LEN, KL + ROPE), jnp.float32), -5.0, 5.0)
    return values.astype(jnp.bfloat16)


def block_levels(key, dims, pieces, least, largest):
    def one(position, shards_of):
        draws = jax.random.uniform(jax.random.fold_in(jax.random.fold_in(key, 6), position), (shards_of,), jnp.float32, least / len(pieces), largest / len(pieces))
        return jnp.repeat(jnp.exp(draws), dims[position] // shards_of).reshape((-1,) + (1,) * (len(dims) - position - 1))

    gain = one(*pieces[0])
    for cut in pieces[1:]:
        gain = gain * one(*cut)
    return gain


def profile(amount, total, most, slope):
    weights = [(1 << 20) // math.isqrt(grade ** slope) + 1 for grade in range(2, amount + 1)]
    rest, holding = total - most - (amount - 1), [1] * (amount - 1)
    while rest > 0:
        candidates = [i for i in range(amount - 1) if holding[i] < most]
        whole, left = sum([weights[i] for i in candidates]), rest
        for i in candidates:
            extra = min(most - holding[i], max(1, left * weights[i] // whole), rest)
            holding[i] = holding[i] + extra
            rest = rest - extra
    return np.array([most] + holding)


def uneven(rng, amount, total, most, skew):
    if amount == 2:
        one = jax.random.randint(rng, (), max(1, total - most), min(most, total - 1) + 1)
        return jnp.stack([one, total - one])
    tallies = jnp.asarray(profile(amount, total, most, skew), jnp.int32)
    couples = (amount - 1) // 2
    donor, receiver = tallies[1:1 + 2 * couples:2], tallies[2:2 + 2 * couples:2]
    margin = jnp.minimum(donor - 1, most - receiver)
    moved = jax.random.randint(jax.random.fold_in(rng, 1), (couples,), 0, 1 << 20) % (margin + 1)
    tallies = tallies.at[1:1 + 2 * couples:2].set(donor - moved).at[2:2 + 2 * couples:2].set(receiver + moved)
    return tallies[jax.random.permutation(jax.random.fold_in(rng, 2), amount)]


def gaussian(stream_key, dims, scale, most, split=(), held_as=jnp.bfloat16):
    result = scale * jax.random.normal(stream_key, dims, jnp.float32)
    if split:
        result = result * block_levels(stream_key, dims, split, -0.22, 0.18)
    return jnp.clip(result, -most, most).astype(held_as)


def setup_inputs(seed: int = 0) -> dict:
    key_of = jax.random.split(jax.random.key(seed), 18)
    return {
        "piece_tokens": gaussian(key_of[0], (PIECE, D), 1.0, 6.0, ((0, 128),)),
        "decode_tokens": gaussian(key_of[1], (DEC, D), 1.0, 6.0, ((0, 128),)),
        "prompt_fill": jax.random.randint(key_of[2], (1,), CACHE // 2, CACHE - PIECE + 1).astype(jnp.int32),
        "decode_fill": uneven(key_of[3], DEC, DEC * DEC_LEN // 2, DEC_LEN - 1, 2).astype(jnp.int32),
        "prompt_cache": draw_prompt_cache(jax.random.fold_in(key_of[17], 71), 0),
        "decode_cache": draw_decode_cache(jax.random.fold_in(key_of[17], 71), 0),
        "input_gain": jnp.clip(1.0 + 0.18 * jax.random.normal(key_of[6], (D,), jnp.float32), 0.1, 1.9),
        "query_gain": jnp.clip(1.0 + 0.18 * jax.random.normal(key_of[7], (QL,), jnp.float32), 0.1, 1.9),
        "latent_gain": jnp.clip(1.0 + 0.18 * jax.random.normal(key_of[8], (KL,), jnp.float32), 0.1, 1.9),
        "query_down": gaussian(key_of[9], (D, QL), D ** -0.5, 0.125, ((1, 4),)),
        "latent_down": gaussian(key_of[10], (D, KL), D ** -0.5, 0.125, ((1, 4),)),
        "rope_down": gaussian(key_of[11], (D, ROPE), D ** -0.5, 0.125),
        "query_up": gaussian(key_of[12], (QL, H * NOPE), QL ** -0.5, 0.21875, ((1, 4),)),
        "qrope_up": gaussian(key_of[13], (QL, H * ROPE), QL ** -0.5, 0.21875, ((1, 4),)),
        "key_up": gaussian(key_of[14], (H, NOPE, KL), KL ** -0.5, 0.25, ((0, 4),)),
        "value_up": gaussian(key_of[15], (H, KL, VD), 0.25, 4.0, ((0, 4),)),
        "out_proj": gaussian(key_of[16], (H * VD, D), 0.25, 4.0, ((0, 4),)),
    }


NEG_FILL = -1e+30
RMS_EPS = 1e-06
THETA = 10000.0

def rms_scale(values, gain_row):
    widened = values.astype(jnp.float32)
    scaled = widened * lax.rsqrt(lax.optimization_barrier(jnp.mean(widened * widened, axis=-1, keepdims=True)) + RMS_EPS) * gain_row.astype(jnp.float32)
    return scaled.astype(jnp.bfloat16)

def rotate(values, places):
    half_width = values.shape[-1] // 2
    inverse = THETA ** (-jnp.arange(half_width, dtype=jnp.float32) / half_width)
    angles = places.astype(jnp.float32)[..., None] * inverse
    first_half = values[..., :half_width].astype(jnp.float32)
    second_half = values[..., half_width:].astype(jnp.float32)
    cosine = jnp.cos(angles)
    sine_part = jnp.sin(angles)
    return jnp.concatenate([first_half * cosine - second_half * sine_part, first_half * sine_part + second_half * cosine], axis=-1).astype(jnp.bfloat16)

def project(tokens, places, input_gain, query_gain, latent_gain, query_down, latent_down, rope_down):
    normed = rms_scale(tokens, input_gain)
    query_comp = jnp.dot(normed, query_down, preferred_element_type=jnp.float32).astype(jnp.bfloat16)
    latent_comp = jnp.dot(normed, latent_down, preferred_element_type=jnp.float32).astype(jnp.bfloat16)
    rope_raw = jnp.dot(normed, rope_down, preferred_element_type=jnp.float32).astype(jnp.bfloat16)
    new_rows = jnp.concatenate([rms_scale(latent_comp, latent_gain), rotate(rope_raw, places)], axis=-1)
    return (rms_scale(query_comp, query_gain), new_rows)

def make_queries(query_lat, places, query_up, qrope_up, key_up):
    row_count = query_lat.shape[0]
    head_count = key_up.shape[0]
    nope_part = jnp.dot(query_lat, query_up, preferred_element_type=jnp.float32).astype(jnp.bfloat16).reshape(row_count, head_count, -1)
    rope_raw = jnp.dot(query_lat, qrope_up, preferred_element_type=jnp.float32).astype(jnp.bfloat16).reshape(row_count, head_count, -1)
    turned = rotate(rope_raw, places[:, None])
    absorbed = jnp.einsum('nhc,hcl->nhl', nope_part.astype(jnp.float32), key_up.astype(jnp.float32)).astype(jnp.bfloat16)
    return (absorbed, turned)

def block_attend(absorbed, turned, key_rows, key_places, query_places, value_up):
    latent_width = value_up.shape[1]
    score_scale = (NOPE + ROPE) ** (-0.5)
    latent_keys = key_rows[:, :latent_width].astype(jnp.float32)
    scores = (jnp.einsum('nhl,sl->nhs', absorbed.astype(jnp.float32), latent_keys) + jnp.einsum('nhr,sr->nhs', turned.astype(jnp.float32), key_rows[:, latent_width:].astype(jnp.float32))) * score_scale
    allowed = key_places[None, None, :] <= query_places[:, None, None]
    scores = jnp.where(allowed, scores, NEG_FILL)
    local_peak = lax.optimization_barrier(jnp.max(scores, axis=-1))
    exp_scores = jnp.where(allowed, jnp.exp(scores - local_peak[..., None]), 0.0)
    weight_sum = lax.optimization_barrier(jnp.sum(exp_scores, axis=-1))
    weights = lax.optimization_barrier(exp_scores.astype(jnp.bfloat16)).astype(jnp.float32)
    mixed_rows = jnp.einsum('nhs,sl->nhl', weights, latent_keys)
    partial_sum = jnp.einsum('nhl,hlv->nhv', mixed_rows, value_up.astype(jnp.float32), precision=lax.Precision.HIGHEST)
    return (partial_sum, weight_sum, local_peak)

def insert_row(cache_rows, new_row, fill_one):
    return lax.dynamic_update_slice(cache_rows, new_row[None], (fill_one.astype(jnp.int32), jnp.zeros((), jnp.int32)))

def project_out(values, out_proj):
    row_count = values.shape[0]
    grouped = values.reshape(row_count, N_TP, -1).astype(jnp.float32)
    weight_groups = out_proj.reshape(N_TP, -1, out_proj.shape[1]).astype(jnp.float32)
    group_out = jnp.einsum('ngk,gkd->ngd', grouped, weight_groups).astype(jnp.bfloat16)
    group_out = lax.optimization_barrier(group_out).astype(jnp.float32)
    return lax.optimization_barrier(jnp.sum(group_out, axis=1)).astype(jnp.bfloat16)

def reference(piece_tokens, decode_tokens, prompt_fill, decode_fill, prompt_cache, decode_cache, input_gain, query_gain, latent_gain, query_down, latent_down, rope_down, query_up, qrope_up, key_up, value_up, out_proj):
    fill_start = prompt_fill[0].astype(jnp.int32)
    piece_places = fill_start + jnp.arange(PIECE, dtype=jnp.int32)
    decode_places = decode_fill.astype(jnp.int32)
    piece_lat, piece_rows = project(piece_tokens, piece_places, input_gain, query_gain, latent_gain, query_down, latent_down, rope_down)
    decode_lat, decode_rows = project(decode_tokens, decode_places, input_gain, query_gain, latent_gain, query_down, latent_down, rope_down)
    piece_absorbed, piece_turned = make_queries(piece_lat, piece_places, query_up, qrope_up, key_up)
    decode_absorbed, decode_turned = make_queries(decode_lat, decode_places, query_up, qrope_up, key_up)
    full_cache = lax.dynamic_update_slice(prompt_cache, piece_rows, (fill_start, jnp.zeros((), jnp.int32)))
    head_count = key_up.shape[0]
    value_width = value_up.shape[2]

    def step(carry, block_index):
        peak_run, numer_run, denom_run = carry
        key_rows = lax.dynamic_slice_in_dim(full_cache, block_index * CACHE_DEV, CACHE_DEV, 0)
        key_places = block_index * CACHE_DEV + jnp.arange(CACHE_DEV, dtype=jnp.int32)
        partial_sum, weight_sum, local_peak = block_attend(piece_absorbed, piece_turned, key_rows, key_places, piece_places, value_up)
        new_peak = jnp.maximum(peak_run, local_peak)
        old_factor = jnp.exp(peak_run - new_peak)
        new_factor = jnp.exp(local_peak - new_peak)
        numer_run = numer_run * old_factor[..., None] + partial_sum * new_factor[..., None]
        denom_run = denom_run * old_factor + weight_sum * new_factor
        return ((new_peak, numer_run, denom_run), None)
    start_carry = (jnp.full((PIECE, head_count), NEG_FILL, jnp.float32), jnp.zeros((PIECE, head_count, value_width), jnp.float32), jnp.zeros((PIECE, head_count), jnp.float32))
    final_carry, unused = lax.scan(step, start_carry, jnp.arange(N_KV, dtype=jnp.int32))
    piece_value = (final_carry[1] / final_carry[2][..., None]).astype(jnp.bfloat16)
    decode_keys = jax.vmap(insert_row)(decode_cache, decode_rows, decode_places)

    def attend_one(absorbed_one, turned_one, keys_one, fill_one):
        key_places = jnp.arange(keys_one.shape[0], dtype=jnp.int32)
        return block_attend(absorbed_one[None], turned_one[None], keys_one, key_places, fill_one[None], value_up)
    decode_part, decode_total, decode_peak = jax.vmap(attend_one)(decode_absorbed, decode_turned, decode_keys, decode_places)
    decode_value = (decode_part[:, 0] / decode_total[:, 0, :, None]).astype(jnp.bfloat16)
    piece_out = project_out(piece_value.reshape(PIECE, -1), out_proj)
    decode_out = project_out(decode_value.reshape(decode_value.shape[0], -1), out_proj)
    return (piece_out, decode_out, piece_rows, decode_rows)
```

```python
import functools
import math

import jax
import jax.numpy as jnp
from jax import lax
from jax.experimental import pallas as pl
from jax.experimental.pallas import tpu as pltpu
from jax.sharding import PartitionSpec as P

NOPE = 64
ROPE = 32
CORES = 2
NEG_FILL = -1e30
RMS_EPS = 1e-06
THETA = 10000.0
SCALE2 = (NOPE + ROPE) ** (-0.5) * math.log2(math.e)
F32 = jnp.float32
BF16 = jnp.bfloat16
MESH = pl.DeviceIdType.MESH


def dot(a, b):
    return jnp.dot(a, b, preferred_element_type=F32)


def dot_t(a, b):
    return lax.dot_general(a, b, (((1,), (1,)), ((), ())), preferred_element_type=F32)


def each(low, high, body):
    if high - low <= 4:
        for i in range(low, high):
            body(i)
    else:
        lax.fori_loop(low, high, lambda i, carry: (body(i), carry)[1], 0)


def far_first(j, count):
    return count // 2 + ((j + 1) // 2) * (1 - 2 * (j % 2))


def kernel(
    n,
    m,
    pt_h,
    dt_h,
    pf_h,
    df_h,
    pc_h,
    dc_h,
    ig_h,
    qg_h,
    lg_h,
    qd_h,
    ld_h,
    rd_h,
    qu_h,
    ru_h,
    ku_h,
    vu_h,
    op_h,
    po_ref,
    do_ref,
    pr_ref,
    dr_ref,
    tok,
    dtok,
    pfill,
    dfill,
    kbuf,
    dbuf,
    ig,
    qg,
    lg,
    qd,
    ld,
    rd,
    qu,
    ru,
    ku,
    vu,
    op,
    x,
    lx,
    qbuf,
    nbuf,
    krt,
    vt,
    csend,
    crecv,
    dbuf_out,
    outs,
    in_sem,
    q_sem,
    l_sem,
    c_sem,
    p_sem,
    d_sem,
    o_sem,
):
    me = lax.axis_index("kv")
    mt = lax.axis_index("tp")
    chips = n // CORES
    ny = math.isqrt(chips)
    nz = chips // ny
    chip = me // CORES
    core = me % CORES
    peer = me + 1 - 2 * core
    z, y = chip // ny, chip % ny
    p = tok.shape[0]
    dd = dtok.shape[0]
    own = lx.shape[1]
    extra = x.shape[0]
    cache = pc_h.shape[1]
    slots = dc_h.shape[2]
    heads = ku.shape[0]
    kl = ku.shape[2]
    key_width = pc_h.shape[0]
    part_q = qd.shape[0]
    part_l = ld.shape[1]
    ql = qu.shape[0]
    block = heads * p
    chunks = len(outs)
    chunk = outs[0].shape[2]
    half_lanes = 64

    pairs = [
        (pt_h, tok),
        (dt_h, dtok),
        (ig_h, ig),
        (qd_h, qd),
        (ld_h, ld),
        (rd_h, rd),
        (pc_h, kbuf.at[0]),
        (ku_h, ku),
        (vu_h, vu),
        (pf_h, pfill),
        (df_h, dfill),
        (qg_h, qg),
        (lg_h, lg),
        (qu_h, qu),
        (ru_h, ru),
        (dc_h, dbuf),
        (op_h, op),
    ]
    loads = [pltpu.make_async_copy(s, d, in_sem.at[i]) for i, (s, d) in enumerate(pairs)]
    for load in loads:
        load.start()
    early, middle, late, last = loads[:6], loads[6:11], loads[11:15], loads[15:]

    barrier = pltpu.get_barrier_semaphore()

    def other(i):
        dz, dy = far_first(i // ny, nz), far_first(i % ny, ny)
        to = ((z + dz) % nz) * ny + (y + dy) % ny
        source = ((z + nz - dz) % nz) * ny + (y + ny - dy) % ny
        return to, source

    def greet(kv, tp):
        pl.semaphore_signal(barrier, inc=1, device_id=(kv, tp), device_id_type=MESH)

    each(0, chips - 1, lambda i: greet(other(i)[0] * CORES + core, mt))
    greet(peer, mt)
    for dt in range(1, m):
        greet(me, lax.rem(mt + dt, m))

    x[...] = jnp.zeros_like(x)
    for load in early:
        load.wait()
    x[0:p, :] = tok[...].astype(F32)
    x[p : p + dd, :] = dtok[...].astype(F32)
    xs = x[...]
    normed = (
        xs * lax.rsqrt(jnp.mean(xs * xs, axis=-1, keepdims=True) + RMS_EPS) * ig[...]
    ).astype(BF16)
    columns = dot_t(normed, qd[...])[0:own]
    lx[mt] = jnp.concatenate([dot(normed, ld[...])[0:own], columns], axis=1).astype(BF16)
    raw = dot_t(normed, rd[...])[0:own].astype(BF16).astype(F32)

    for load in middle:
        load.wait()
    fill = pfill[...]
    row = lax.broadcasted_iota(jnp.int32, (own, 1), 0)
    places = fill + me * p + row
    for b in range(dd):
        places = jnp.where(row == p + b, dfill[b : b + 1, :], places)
    half = ROPE // 2
    lane = lax.broadcasted_iota(jnp.int32, (1, heads * ROPE), 1)
    frequency = jnp.zeros((1, heads * ROPE), F32)
    for i in range(half):
        frequency = jnp.where(lane % half == i, THETA ** (-i / half), frequency)
    angles = places.astype(F32) * frequency
    cosine = jnp.cos(angles)
    sine = jnp.sin(angles)
    cos_own = cosine[:, 0:half]
    sin_own = sine[:, 0:half]
    first, second = raw[:, 0:half], raw[:, half:ROPE]
    new_rope = jnp.concatenate(
        [first * cos_own - second * sin_own, first * sin_own + second * cos_own], axis=1
    )

    key_up = ku[...].reshape(heads * NOPE, kl)
    value_up = vu[...].reshape(vu.shape[0] * vu.shape[1], kl)

    def expand(slot, owner):
        at = slice(slot * cache, (slot + 1) * cache)
        latent_t = kbuf[slot, 0:kl]
        rope_t = kbuf[slot, kl:key_width]
        krt[0 : heads * NOPE, at] = dot(key_up, latent_t).astype(BF16)
        vt[:, at] = dot(value_up, latent_t).astype(BF16)
        sub = lax.broadcasted_iota(jnp.int32, (ROPE, cache), 0)
        place = owner * cache + lax.broadcasted_iota(jnp.int32, (ROPE, cache), 1)
        bias = jnp.where((sub == 0) & (place >= fill), NEG_FILL, 0.0).astype(BF16)
        krt[heads * NOPE :, at] = jnp.concatenate([rope_t, bias, rope_t, bias], axis=0)

    expand(0, me)

    pl.semaphore_wait(barrier, chips - 1 + 1 + m - 1)

    l_copies = []
    for dt in range(1, m):
        copy = pltpu.make_async_remote_copy(
            src_ref=lx.at[mt],
            dst_ref=lx.at[mt],
            send_sem=l_sem.at[0, dt],
            recv_sem=l_sem.at[1, dt],
            device_id=(me, lax.rem(mt + dt, m)),
            device_id_type=MESH,
        )
        copy.start()
        l_copies.append(copy)

    def peer_copy(src, dst, index):
        return pltpu.make_async_remote_copy(
            src_ref=src,
            dst_ref=dst,
            send_sem=p_sem.at[0, index],
            recv_sem=p_sem.at[1, index],
            device_id=(peer, mt),
            device_id_type=MESH,
        )

    cache_copy = peer_copy(kbuf.at[0], kbuf.at[1], 0)
    cache_copy.start()
    for load in late:
        load.wait()
    gains = qg[...].reshape(1, ql)

    for copy in l_copies:
        copy.wait_recv()
    parts = [lx[s, :, part_l:].astype(F32) for s in range(m)]
    square = sum(jnp.sum(v * v, axis=-1, keepdims=True) for v in parts)
    scale = lax.rsqrt(square / ql + RMS_EPS)
    nope = jnp.zeros((own, qu.shape[1]), F32)
    turn = jnp.zeros((own, ru.shape[1]), F32)
    for s in range(m):
        lat = (parts[s] * scale * gains[:, s * part_q : (s + 1) * part_q]).astype(BF16)
        nope += dot(lat, qu[s * part_q : (s + 1) * part_q, :])
        turn += dot(lat, ru[s * part_q : (s + 1) * part_q, :])
    nope = nope.astype(BF16).astype(F32)
    turn = turn.astype(BF16).astype(F32)
    turned_axis = heads * ROPE
    above = pltpu.roll(turn, turned_axis - half, 1)
    below = pltpu.roll(turn, half, 1)
    turned = turn * cosine + jnp.where(lane % ROPE < half, -above, below) * sine
    blocks = []
    for h in range(heads):
        base = half_lanes * (1 - h % 2)
        shift = (base - h * ROPE) % 128
        moved = pltpu.roll(turned, shift, 1) if shift else turned
        tile = nope[:, (h // 2) * 128 : (h // 2 + 1) * 128]
        rest = jnp.where(lane < base + ROPE, moved, jnp.where(lane == base + ROPE, 1.0, 0.0))
        blocks.append(jnp.where((lane >= base) & (lane < base + half_lanes), rest, tile))
    message = jnp.concatenate([v[0:p] for v in blocks], axis=0).astype(BF16)
    own_rows = pl.ds(pl.multiple_of(chip * block, block), block)
    qbuf[own_rows, :] = message

    def rows_of(ref, index):
        return ref.at[pl.ds(pl.multiple_of(index * block, block), block)]

    def query_copy(i):
        to, source = other(i)
        return pltpu.make_async_remote_copy(
            src_ref=rows_of(qbuf, chip),
            dst_ref=rows_of(qbuf, chip),
            send_sem=q_sem.at[0, i],
            recv_sem=q_sem.at[1, i],
            device_id=(to * CORES + core, mt),
            device_id_type=MESH,
        )

    def query_arrival(i):
        to, source = other(i)
        return pltpu.make_async_remote_copy(
            src_ref=rows_of(qbuf, source),
            dst_ref=rows_of(qbuf, source),
            send_sem=q_sem.at[0, i],
            recv_sem=q_sem.at[1, i],
            device_id=(to * CORES + core, mt),
            device_id_type=MESH,
        )

    each(0, chips - 1, lambda i: query_copy(i).start())

    latent = jnp.concatenate([lx[s, :, 0:part_l].astype(F32) for s in range(m)], axis=1)
    latent = (
        latent * lax.rsqrt(jnp.mean(latent * latent, axis=-1, keepdims=True) + RMS_EPS) * lg[...]
    )
    new_rows = jnp.concatenate([latent, new_rope], axis=1)
    pr_ref[...] = new_rows[0:p].astype(BF16)
    dr_ref[...] = new_rows[p : p + dd].astype(BF16)
    new_bf = jnp.concatenate([new_rows, jnp.zeros((extra - own, key_width), F32)], axis=0)
    new_bf = new_bf.astype(BF16)
    nbuf[0] = new_bf
    rows_copy = peer_copy(nbuf.at[0], nbuf.at[1], 1)
    rows_copy.start()

    cache_copy.wait_recv()
    expand(1, peer)

    for load in last:
        load.wait()
    new_latent, new_key = new_bf[:, 0:kl], new_bf[:, kl:key_width]
    head_row = lax.broadcasted_iota(jnp.int32, (heads, heads * NOPE), 0)
    head_lane = lax.broadcasted_iota(jnp.int32, (heads, heads * NOPE), 1) // NOPE
    dvalues = []
    for b in range(dd):
        at = slice(p + b, p + b + 1)
        nope_rows = jnp.concatenate([nope[at]] * heads, axis=0)
        nope_rows = jnp.where(head_row == head_lane, nope_rows, 0.0).astype(BF16)
        qa = dot(nope_rows, key_up).astype(BF16)
        qt = jnp.concatenate(
            [turned[at, h * ROPE : (h + 1) * ROPE] for h in range(heads)], axis=0
        ).astype(BF16)
        ds = dot(qa, dbuf[b, 0:kl]) + dot(qt, dbuf[b, kl:key_width])
        df = dot_t(qa, new_latent) + dot_t(qt, new_key)
        dk = lax.broadcasted_iota(jnp.int32, ds.shape, 1)
        ds = jnp.where(dk < dfill[b : b + 1, :], ds, NEG_FILL)
        fk = lax.broadcasted_iota(jnp.int32, df.shape, 1)
        df = jnp.where(fk == p + b, df, NEG_FILL)
        dpeak = jnp.maximum(
            jnp.max(ds, axis=-1, keepdims=True), jnp.max(df, axis=-1, keepdims=True)
        )
        dw = jnp.exp2((ds - dpeak) * SCALE2)
        fw = jnp.exp2((df - dpeak) * SCALE2)
        dtotal = jnp.sum(dw, axis=-1, keepdims=True) + jnp.sum(fw, axis=-1, keepdims=True)
        dmix = dot_t(dw.astype(BF16), dbuf[b, 0:kl]) + dot(fw.astype(BF16), new_latent)
        dval = dot_t(dmix.astype(BF16), value_up) / dtotal
        dvalues.append(
            jnp.sum(jnp.where(head_row == head_lane, dval, 0.0), axis=0, keepdims=True)
        )

    def row_copy(buf, sem, dt):
        return pltpu.make_async_remote_copy(
            src_ref=buf.at[mt],
            dst_ref=buf.at[mt],
            send_sem=sem.at[0, dt],
            recv_sem=sem.at[1, dt],
            device_id=(me, lax.rem(mt + dt, m)),
            device_id_type=MESH,
        )

    dbuf_out[mt] = dot(jnp.concatenate(dvalues, axis=0).astype(BF16), op[...]).astype(BF16)
    o_copies = [row_copy(dbuf_out, d_sem, dt) for dt in range(1, m)]
    for copy in o_copies:
        copy.start()

    rows_copy.wait_recv()
    fresh = nbuf[...].reshape(2 * extra, key_width)
    fresh_rope = fresh[:, kl:key_width]
    gap = jnp.zeros((2 * extra, half_lanes - ROPE), BF16)
    fresh_key = jnp.concatenate(
        [dot_t(fresh[:, 0:kl], key_up).astype(BF16), fresh_rope, gap, fresh_rope, gap], axis=1
    )
    fresh_value = dot_t(fresh[:, 0:kl], value_up).astype(BF16)

    tile_rows = min(256, chips * block)
    lane_t = lax.broadcasted_iota(jnp.int32, (tile_rows, 128), 1)
    row_t = lax.broadcasted_iota(jnp.int32, (tile_rows, 128), 0)
    head_t = (row_t % block) // p
    low_t = lane_t < half_lanes
    even_t = head_t % 2 == 0
    is_nope = low_t == even_t
    pick = lambda mask: jnp.where(mask, 1.0, 0.0).astype(BF16)
    mask0 = pick(is_nope & (head_t < 2))
    mask1 = pick(is_nope & (head_t >= 2))
    mask_r = pick(jnp.logical_not(is_nope))
    frow = lax.broadcasted_iota(jnp.int32, (tile_rows, 2 * extra), 0)
    fcol = lax.broadcasted_iota(jnp.int32, (tile_rows, 2 * extra), 1)
    fplace = jnp.where(fcol < extra, me * p + fcol, peer * p + fcol - extra)
    freal = (fcol % extra) < p

    each(0, chips - 1, lambda i: query_arrival(i).wait_recv())

    for r0 in range(0, chips * block, tile_rows):
        rows = slice(r0, r0 + tile_rows)
        q = qbuf[rows, :]
        q = jnp.concatenate([q * mask0, q * mask1, q * mask_r], axis=1)
        s = dot(q, krt[...])
        sf = dot_t(q, fresh_key)
        qplace = ((r0 + frow) // block * CORES + core) * p + frow % p
        sf = jnp.where(freal & (fplace <= qplace), sf, NEG_FILL)
        peak = jnp.maximum(jnp.max(s, axis=-1, keepdims=True), jnp.max(sf, axis=-1, keepdims=True))
        w = jnp.exp2((s - peak) * SCALE2)
        wf = jnp.exp2((sf - peak) * SCALE2)
        total = jnp.sum(w, axis=-1, keepdims=True) + jnp.sum(wf, axis=-1, keepdims=True)
        o = dot_t(w.astype(BF16), vt[...]) + dot(wf.astype(BF16), fresh_value)
        o = jnp.where(head_t < 2, o[:, 0:128], o[:, 128:256])
        o = jnp.where(even_t, o, pltpu.roll(o, half_lanes, 1))
        level = peak * SCALE2 + jnp.log2(total)
        high = level.astype(BF16).astype(F32)
        mid = (level - high).astype(BF16).astype(F32)
        stats = jnp.where(lane_t == half_lanes, high, level - high - mid)
        stats = jnp.where(lane_t == half_lanes + 1, mid, stats)
        csend[rows, :] = jnp.where(low_t, o * (1.0 / total), stats).astype(BF16)

    def value_copy(i):
        to, source = other(i)
        return pltpu.make_async_remote_copy(
            src_ref=rows_of(csend, to),
            dst_ref=rows_of(crecv, chip),
            send_sem=c_sem.at[0, i],
            recv_sem=c_sem.at[1, i],
            device_id=(to * CORES + core, mt),
            device_id_type=MESH,
        )

    def value_arrival(i):
        to, source = other(i)
        return pltpu.make_async_remote_copy(
            src_ref=rows_of(csend, to),
            dst_ref=rows_of(crecv, source),
            send_sem=c_sem.at[0, i],
            recv_sem=c_sem.at[1, i],
            device_id=(to * CORES + core, mt),
            device_id_type=MESH,
        )

    each(0, chips - 1, lambda i: value_copy(i).start())
    crecv[own_rows, :] = csend[own_rows, :]

    for copy in o_copies:
        copy.wait_recv()
    do_ref[...] = sum(dbuf_out[s].astype(F32) for s in range(m)).astype(BF16)
    stat_row = lax.broadcasted_iota(jnp.int32, (128, 128), 0)
    summing = pick((stat_row >= half_lanes) & (stat_row < half_lanes + 3))

    each(0, chips - 1, lambda i: value_arrival(i).wait_recv())
    arrived = crecv[...]
    levels = dot(arrived, summing).reshape(chips, block, 128)
    arrived = arrived.astype(F32).reshape(chips, block, 128)
    top = jnp.max(levels, axis=0, keepdims=True)
    share = jnp.exp2(levels - top)
    value = jnp.sum(arrived * share, axis=0) / jnp.sum(share, axis=0)
    low = lax.broadcasted_iota(jnp.int32, (p, 128), 1) < half_lanes
    values = []
    for h in range(0, heads, 2):
        right = pltpu.roll(value[(h + 1) * p : (h + 2) * p], half_lanes, 1)
        values.append(jnp.where(low, value[h * p : (h + 1) * p], right))
    values = jnp.concatenate(values, axis=1).astype(BF16)
    p_copies = []
    for c in range(chunks):
        obuf = outs[c]
        obuf[mt] = dot(values, op[:, c * chunk : (c + 1) * chunk]).astype(BF16)
        for dt in range(1, m):
            copy = row_copy(obuf, o_sem.at[c], dt)
            copy.start()
            p_copies.append(copy)
    for c in range(chunks):
        for copy in p_copies[c * (m - 1) : (c + 1) * (m - 1)]:
            copy.wait_recv()
        out = sum(outs[c][s].astype(F32) for s in range(m))
        po_ref[:, c * chunk : (c + 1) * chunk] = out.astype(BF16)
    each(0, chips - 1, lambda i: query_copy(i).wait_send())
    each(0, chips - 1, lambda i: value_copy(i).wait_send())
    for copy in l_copies + [cache_copy, rows_copy] + o_copies + p_copies:
        copy.wait_send()


def put_out(*refs):
    count = len(refs) // 2
    sem = refs[-1]
    copies = [
        pltpu.make_async_copy(refs[i], refs[count + i], sem.at[i]) for i in range(count)
    ]
    for copy in copies:
        copy.start()
    for copy in copies:
        copy.wait()


def local(n, m, *args):
    (pt, dt, pfill, dfill, pc, dc, ig, qg, lg, qd, ld, rd, qu, ru, ku, vu, op) = args
    p, width = pt.shape
    dd = dt.shape[0]
    own = -(-(p + dd) // 8) * 8
    extra = 16
    heads, nd, kl = ku.shape
    block = heads * p
    chips = n // CORES
    chunks = 2
    any_spec = pl.BlockSpec(memory_space=pltpu.HBM)
    vmem = pl.BlockSpec(memory_space=pltpu.VMEM)
    ig, lg = ig[None], lg[None]
    pfill, dfill = pfill[None], dfill[:, None]
    pc, qd, rd = pc.T, qd.T, rd.T
    dc, vu = jnp.swapaxes(dc, 1, 2), jnp.swapaxes(vu, 1, 2)
    cache = pc.shape[1]
    like = lambda a: pltpu.VMEM(a.shape, a.dtype)
    scratch = [
        *[like(a) for a in (pt, dt, pfill, dfill)],
        pltpu.VMEM((2, *pc.shape), BF16),
        *[like(a) for a in (dc, ig, qg, lg)],
        *[like(a) for a in (qd, ld, rd, qu, ru, ku, vu, op)],
        pltpu.VMEM((extra, width), F32),
        pltpu.VMEM((m, own, ld.shape[1] + qd.shape[0]), BF16),
        pltpu.VMEM((chips * block, 128), BF16),
        pltpu.VMEM((2, extra, pc.shape[0]), BF16),
        pltpu.VMEM((heads * nd + 128, 2 * cache), BF16),
        pltpu.VMEM((heads * nd, 2 * cache), BF16),
        pltpu.VMEM((chips * block, 128), BF16),
        pltpu.VMEM((chips * block, 128), BF16),
        pltpu.VMEM((m, dd, width), BF16),
        [pltpu.VMEM((m, p, width // chunks), BF16)] * chunks,
        pltpu.SemaphoreType.DMA((17,)),
        pltpu.SemaphoreType.DMA((2, chips)),
        pltpu.SemaphoreType.DMA((2, m)),
        pltpu.SemaphoreType.DMA((2, chips)),
        pltpu.SemaphoreType.DMA((2, 2)),
        pltpu.SemaphoreType.DMA((2, m)),
        pltpu.SemaphoreType.DMA((chunks, 2, m)),
    ]
    held = pl.pallas_call(
        functools.partial(kernel, n, m),
        out_shape=(
            pltpu.VMEM((p, width), BF16),
            pltpu.VMEM((dd, width), BF16),
            pltpu.VMEM((p, pc.shape[0]), BF16),
            pltpu.VMEM((dd, pc.shape[0]), BF16),
        ),
        in_specs=[any_spec] * 17,
        out_specs=(vmem,) * 4,
        scratch_shapes=scratch,
        compiler_params=pltpu.CompilerParams(
            collective_id=0, has_side_effects=True, vmem_limit_bytes=60 * 1024 * 1024
        ),
    )(pt, dt, pfill, dfill, pc, dc, ig, qg, lg, qd, ld, rd, qu, ru, ku, vu, op)
    return pl.pallas_call(
        put_out,
        out_shape=tuple(jax.ShapeDtypeStruct(a.shape, a.dtype) for a in held),
        in_specs=[vmem] * len(held),
        out_specs=(any_spec,) * len(held),
        scratch_shapes=[pltpu.SemaphoreType.DMA((len(held),))],
        compiler_params=pltpu.CompilerParams(vmem_limit_bytes=1024 * 1024),
    )(*held)


def solution(mesh):
    placed = (
        P("kv", None),
        P("kv", None),
        P(),
        P("kv"),
        P("kv", None),
        P("kv", None, None),
        P(),
        P(),
        P(),
        P(None, "tp"),
        P(None, "tp"),
        P(),
        P(None, "tp"),
        P(None, "tp"),
        P("tp", None, None),
        P("tp", None, None),
        P("tp", None),
    )
    return jax.shard_map(
        functools.partial(local, mesh.shape["kv"], mesh.shape["tp"]),
        mesh=mesh,
        in_specs=placed,
        out_specs=(P("kv", None), P("kv", None), P("kv", None), P("kv", None)),
        check_vma=False,
    )
```

```python
import functools
import math

import jax
import jax.numpy as jnp
from jax import lax
from jax.experimental import pallas as pl
from jax.experimental.pallas import tpu as pltpu
from jax.sharding import PartitionSpec as P

NOPE = 64
ROPE = 32
CORES = 2
NEG_FILL = -1e30
RMS_EPS = 1e-06
THETA = 10000.0
SCALE2 = (NOPE + ROPE) ** (-0.5) * math.log2(math.e)
F32 = jnp.float32
BF16 = jnp.bfloat16
MESH = pl.DeviceIdType.MESH


def dot(a, b):
    return jnp.dot(a, b, preferred_element_type=F32)


def dot_t(a, b):
    return lax.dot_general(a, b, (((1,), (1,)), ((), ())), preferred_element_type=F32)


def each(low, high, body):
    if high - low <= 4:
        for i in range(low, high):
            body(i)
    else:
        lax.fori_loop(low, high, lambda i, carry: (body(i), carry)[1], 0)


def far_first(j, count):
    return count // 2 + ((j + 1) // 2) * (1 - 2 * (j % 2))


def kernel(
    n,
    m,
    pt_h,
    dt_h,
    pf_h,
    df_h,
    pc_h,
    dc_h,
    ig_h,
    qg_h,
    lg_h,
    qd_h,
    ld_h,
    rd_h,
    qu_h,
    ru_h,
    ku_h,
    vu_h,
    op_h,
    po_ref,
    do_ref,
    pr_ref,
    dr_ref,
    tok,
    dtok,
    pfill,
    dfill,
    kbuf,
    dbuf,
    ig,
    qg,
    lg,
    qd,
    ld,
    rd,
    qu,
    ru,
    ku,
    vu,
    op,
    x,
    lx,
    qbuf,
    nbuf,
    krt,
    vt,
    csend,
    crecv,
    dbuf_out,
    outs,
    line_sem,
    in_sem,
    q_sem,
    l_sem,
    c_sem,
    p_sem,
    d_sem,
    o_sem,
):
    me = lax.axis_index("kv")
    mt = lax.axis_index("tp")
    chips = n // CORES
    ny = math.isqrt(chips)
    nz = chips // ny
    chip = me // CORES
    core = me % CORES
    peer = me + 1 - 2 * core
    z, y = chip // ny, chip % ny
    p = tok.shape[0]
    dd = dtok.shape[0]
    own = lx.shape[1]
    extra = x.shape[0]
    cache = pc_h.shape[1]
    slots = dc_h.shape[2]
    heads = ku.shape[0]
    kl = ku.shape[2]
    key_width = pc_h.shape[0]
    part_q = qd.shape[0]
    part_l = ld.shape[1]
    ql = qu.shape[0]
    block = heads * p
    chunks = len(outs)
    chunk = outs[0].shape[2]
    half_lanes = 64

    pairs = [
        (pt_h, tok),
        (dt_h, dtok),
        (ig_h, ig),
        (qd_h, qd),
        (ld_h, ld),
        (rd_h, rd),
        (pc_h, kbuf.at[0]),
        (ku_h, ku),
        (vu_h, vu),
        (pf_h, pfill),
        (df_h, dfill),
        (qg_h, qg),
        (lg_h, lg),
        (qu_h, qu),
        (ru_h, ru),
        (dc_h, dbuf),
        (op_h, op),
    ]
    loads = [pltpu.make_async_copy(s, d, in_sem.at[i]) for i, (s, d) in enumerate(pairs)]
    for load in loads:
        load.start()
    early, middle, late, last = loads[:6], loads[6:11], loads[11:15], loads[15:]

    barrier = pltpu.get_barrier_semaphore()

    def other(i):
        dz, dy = far_first(i // ny, nz), far_first(i % ny, ny)
        to = ((z + dz) % nz) * ny + (y + dy) % ny
        source = ((z + nz - dz) % nz) * ny + (y + ny - dy) % ny
        return to, source

    def greet(kv, tp):
        pl.semaphore_signal(barrier, inc=1, device_id=(kv, tp), device_id_type=MESH)

    def along_z(dz):
        return (((z + dz) % nz) * ny + y) * CORES + core

    each(1, nz, lambda dz: greet(along_z(dz), mt))
    each(1, ny, lambda dy: greet((z * ny + (y + dy) % ny) * CORES + core, mt))
    greet(peer, mt)
    for dt in range(1, m):
        greet(me, lax.rem(mt + dt, m))

    x[...] = jnp.zeros_like(x)
    for load in early:
        load.wait()
    x[0:p, :] = tok[...].astype(F32)
    x[p : p + dd, :] = dtok[...].astype(F32)
    xs = x[...]
    normed = (
        xs * lax.rsqrt(jnp.mean(xs * xs, axis=-1, keepdims=True) + RMS_EPS) * ig[...]
    ).astype(BF16)
    columns = dot_t(normed, qd[...])[0:own]
    lx[mt] = jnp.concatenate([dot(normed, ld[...])[0:own], columns], axis=1).astype(BF16)
    raw = dot_t(normed, rd[...])[0:own].astype(BF16).astype(F32)

    for load in middle:
        load.wait()
    fill = pfill[0]
    row = lax.broadcasted_iota(jnp.int32, (own, 1), 0)
    places = fill + me * p + row
    for b in range(dd):
        places = jnp.where(row == p + b, dfill[b], places)
    half = ROPE // 2
    lane = lax.broadcasted_iota(jnp.int32, (1, heads * ROPE), 1)
    frequency = jnp.zeros((1, heads * ROPE), F32)
    for i in range(half):
        frequency = jnp.where(lane % half == i, THETA ** (-i / half), frequency)
    angles = places.astype(F32) * frequency
    cosine = jnp.cos(angles)
    sine = jnp.sin(angles)
    cos_own = cosine[:, 0:half]
    sin_own = sine[:, 0:half]
    first, second = raw[:, 0:half], raw[:, half:ROPE]
    new_rope = jnp.concatenate(
        [first * cos_own - second * sin_own, first * sin_own + second * cos_own], axis=1
    )

    key_up = ku[...].reshape(heads * NOPE, kl)
    value_up = vu[...].reshape(vu.shape[0] * vu.shape[1], kl)

    def expand(slot, owner):
        at = slice(slot * cache, (slot + 1) * cache)
        latent_t = kbuf[slot, 0:kl]
        rope_t = kbuf[slot, kl:key_width]
        krt[0 : heads * NOPE, at] = dot(key_up, latent_t).astype(BF16)
        vt[:, at] = dot(value_up, latent_t).astype(BF16)
        sub = lax.broadcasted_iota(jnp.int32, (ROPE, cache), 0)
        place = owner * cache + lax.broadcasted_iota(jnp.int32, (ROPE, cache), 1)
        bias = jnp.where((sub == 0) & (place >= fill), NEG_FILL, 0.0).astype(BF16)
        krt[heads * NOPE :, at] = jnp.concatenate([rope_t, bias, rope_t, bias], axis=0)

    expand(0, me)

    pl.semaphore_wait(barrier, nz - 1 + ny - 1 + 1 + m - 1)

    def vouch(dz):
        pl.semaphore_signal(line_sem, inc=1, device_id=(along_z(dz), mt), device_id_type=MESH)

    each(1, nz, vouch)

    l_copies = []
    for dt in range(1, m):
        copy = pltpu.make_async_remote_copy(
            src_ref=lx.at[mt],
            dst_ref=lx.at[mt],
            send_sem=l_sem.at[0, dt],
            recv_sem=l_sem.at[1, dt],
            device_id=(me, lax.rem(mt + dt, m)),
            device_id_type=MESH,
        )
        copy.start()
        l_copies.append(copy)

    def peer_copy(src, dst, index):
        return pltpu.make_async_remote_copy(
            src_ref=src,
            dst_ref=dst,
            send_sem=p_sem.at[0, index],
            recv_sem=p_sem.at[1, index],
            device_id=(peer, mt),
            device_id_type=MESH,
        )

    cache_copy = peer_copy(kbuf.at[0], kbuf.at[1], 0)
    cache_copy.start()
    for load in late:
        load.wait()
    gains = qg[...].reshape(1, ql)

    for copy in l_copies:
        copy.wait_recv()
    parts = [lx[s, :, part_l:].astype(F32) for s in range(m)]
    square = sum(jnp.sum(v * v, axis=-1, keepdims=True) for v in parts)
    scale = lax.rsqrt(square / ql + RMS_EPS)
    nope = jnp.zeros((own, qu.shape[1]), F32)
    turn = jnp.zeros((own, ru.shape[1]), F32)
    for s in range(m):
        lat = (parts[s] * scale * gains[:, s * part_q : (s + 1) * part_q]).astype(BF16)
        nope += dot(lat, qu[s * part_q : (s + 1) * part_q, :])
        turn += dot(lat, ru[s * part_q : (s + 1) * part_q, :])
    nope = nope.astype(BF16).astype(F32)
    turn = turn.astype(BF16).astype(F32)
    turned_axis = heads * ROPE
    above = pltpu.roll(turn, turned_axis - half, 1)
    below = pltpu.roll(turn, half, 1)
    turned = turn * cosine + jnp.where(lane % ROPE < half, -above, below) * sine
    blocks = []
    for h in range(heads):
        base = half_lanes * (1 - h % 2)
        shift = (base - h * ROPE) % 128
        moved = pltpu.roll(turned, shift, 1) if shift else turned
        tile = nope[:, (h // 2) * 128 : (h // 2 + 1) * 128]
        rest = jnp.where(lane < base + ROPE, moved, jnp.where(lane == base + ROPE, 1.0, 0.0))
        blocks.append(jnp.where((lane >= base) & (lane < base + half_lanes), rest, tile))
    message = jnp.concatenate([v[0:p] for v in blocks], axis=0).astype(BF16)
    own_rows = pl.ds(pl.multiple_of(chip * block, block), block)
    qbuf[own_rows, :] = message

    def rows_of(ref, index):
        return ref.at[pl.ds(pl.multiple_of(index * block, block), block)]

    def query_copy(i):
        to, source = other(i)
        return pltpu.make_async_remote_copy(
            src_ref=rows_of(qbuf, chip),
            dst_ref=rows_of(qbuf, chip),
            send_sem=q_sem.at[0, i],
            recv_sem=q_sem.at[1, i],
            device_id=(to * CORES + core, mt),
            device_id_type=MESH,
        )

    def query_arrival(i):
        to, source = other(i)
        return pltpu.make_async_remote_copy(
            src_ref=rows_of(qbuf, source),
            dst_ref=rows_of(qbuf, source),
            send_sem=q_sem.at[0, i],
            recv_sem=q_sem.at[1, i],
            device_id=(to * CORES + core, mt),
            device_id_type=MESH,
        )

    pl.semaphore_wait(line_sem, nz - 1)
    each(0, chips - 1, lambda i: query_copy(i).start())

    latent = jnp.concatenate([lx[s, :, 0:part_l].astype(F32) for s in range(m)], axis=1)
    latent = (
        latent * lax.rsqrt(jnp.mean(latent * latent, axis=-1, keepdims=True) + RMS_EPS) * lg[...]
    )
    new_rows = jnp.concatenate([latent, new_rope], axis=1)
    pr_ref[...] = new_rows[0:p].astype(BF16)
    dr_ref[...] = new_rows[p : p + dd].astype(BF16)
    new_bf = jnp.concatenate([new_rows, jnp.zeros((extra - own, key_width), F32)], axis=0)
    new_bf = new_bf.astype(BF16)
    nbuf[0] = new_bf
    rows_copy = peer_copy(nbuf.at[0], nbuf.at[1], 1)
    rows_copy.start()

    cache_copy.wait_recv()
    expand(1, peer)

    for load in last:
        load.wait()
    new_latent, new_key = new_bf[:, 0:kl], new_bf[:, kl:key_width]
    head_row = lax.broadcasted_iota(jnp.int32, (heads, heads * NOPE), 0)
    head_lane = lax.broadcasted_iota(jnp.int32, (heads, heads * NOPE), 1) // NOPE
    dvalues = []
    for b in range(dd):
        at = slice(p + b, p + b + 1)
        nope_rows = jnp.concatenate([nope[at]] * heads, axis=0)
        nope_rows = jnp.where(head_row == head_lane, nope_rows, 0.0).astype(BF16)
        qa = dot(nope_rows, key_up).astype(BF16)
        qt = jnp.concatenate(
            [turned[at, h * ROPE : (h + 1) * ROPE] for h in range(heads)], axis=0
        ).astype(BF16)
        ds = dot(qa, dbuf[b, 0:kl]) + dot(qt, dbuf[b, kl:key_width])
        df = dot_t(qa, new_latent) + dot_t(qt, new_key)
        dk = lax.broadcasted_iota(jnp.int32, ds.shape, 1)
        ds = jnp.where(dk < dfill[b], ds, NEG_FILL)
        fk = lax.broadcasted_iota(jnp.int32, df.shape, 1)
        df = jnp.where(fk == p + b, df, NEG_FILL)
        dpeak = jnp.maximum(
            jnp.max(ds, axis=-1, keepdims=True), jnp.max(df, axis=-1, keepdims=True)
        )
        dw = jnp.exp2((ds - dpeak) * SCALE2)
        fw = jnp.exp2((df - dpeak) * SCALE2)
        dtotal = jnp.sum(dw, axis=-1, keepdims=True) + jnp.sum(fw, axis=-1, keepdims=True)
        dmix = dot_t(dw.astype(BF16), dbuf[b, 0:kl]) + dot(fw.astype(BF16), new_latent)
        dval = dot_t(dmix.astype(BF16), value_up) / dtotal
        dvalues.append(
            jnp.sum(jnp.where(head_row == head_lane, dval, 0.0), axis=0, keepdims=True)
        )

    def row_copy(buf, sem, dt):
        return pltpu.make_async_remote_copy(
            src_ref=buf.at[mt],
            dst_ref=buf.at[mt],
            send_sem=sem.at[0, dt],
            recv_sem=sem.at[1, dt],
            device_id=(me, lax.rem(mt + dt, m)),
            device_id_type=MESH,
        )

    dbuf_out[mt] = dot(jnp.concatenate(dvalues, axis=0).astype(BF16), op[...]).astype(BF16)
    o_copies = [row_copy(dbuf_out, d_sem, dt) for dt in range(1, m)]
    for copy in o_copies:
        copy.start()

    rows_copy.wait_recv()
    fresh = nbuf[...].reshape(2 * extra, key_width)
    fresh_rope = fresh[:, kl:key_width]
    gap = jnp.zeros((2 * extra, half_lanes - ROPE), BF16)
    fresh_key = jnp.concatenate(
        [dot_t(fresh[:, 0:kl], key_up).astype(BF16), fresh_rope, gap, fresh_rope, gap], axis=1
    )
    fresh_value = dot_t(fresh[:, 0:kl], value_up).astype(BF16)

    tile_rows = min(256, chips * block)
    lane_t = lax.broadcasted_iota(jnp.int32, (tile_rows, 128), 1)
    row_t = lax.broadcasted_iota(jnp.int32, (tile_rows, 128), 0)
    head_t = (row_t % block) // p
    low_t = lane_t < half_lanes
    even_t = head_t % 2 == 0
    is_nope = low_t == even_t
    pick = lambda mask: jnp.where(mask, 1.0, 0.0).astype(BF16)
    mask0 = pick(is_nope & (head_t < 2))
    mask1 = pick(is_nope & (head_t >= 2))
    mask_r = pick(jnp.logical_not(is_nope))
    frow = lax.broadcasted_iota(jnp.int32, (tile_rows, 2 * extra), 0)
    fcol = lax.broadcasted_iota(jnp.int32, (tile_rows, 2 * extra), 1)
    fplace = jnp.where(fcol < extra, me * p + fcol, peer * p + fcol - extra)
    freal = (fcol % extra) < p

    each(0, chips - 1, lambda i: query_arrival(i).wait_recv())

    for r0 in range(0, chips * block, tile_rows):
        rows = slice(r0, r0 + tile_rows)
        q = qbuf[rows, :]
        q = jnp.concatenate([q * mask0, q * mask1, q * mask_r], axis=1)
        s = dot(q, krt[...])
        sf = dot_t(q, fresh_key)
        qplace = ((r0 + frow) // block * CORES + core) * p + frow % p
        sf = jnp.where(freal & (fplace <= qplace), sf, NEG_FILL)
        peak = jnp.maximum(jnp.max(s, axis=-1, keepdims=True), jnp.max(sf, axis=-1, keepdims=True))
        w = jnp.exp2((s - peak) * SCALE2)
        wf = jnp.exp2((sf - peak) * SCALE2)
        total = jnp.sum(w, axis=-1, keepdims=True) + jnp.sum(wf, axis=-1, keepdims=True)
        o = dot_t(w.astype(BF16), vt[...]) + dot(wf.astype(BF16), fresh_value)
        o = jnp.where(head_t < 2, o[:, 0:128], o[:, 128:256])
        o = jnp.where(even_t, o, pltpu.roll(o, half_lanes, 1))
        level = peak * SCALE2 + jnp.log2(total)
        high = level.astype(BF16).astype(F32)
        mid = (level - high).astype(BF16).astype(F32)
        stats = jnp.where(lane_t == half_lanes, high, level - high - mid)
        stats = jnp.where(lane_t == half_lanes + 1, mid, stats)
        csend[rows, :] = jnp.where(low_t, o * (1.0 / total), stats).astype(BF16)

    def value_copy(i):
        to, source = other(i)
        return pltpu.make_async_remote_copy(
            src_ref=rows_of(csend, to),
            dst_ref=rows_of(crecv, chip),
            send_sem=c_sem.at[0, i],
            recv_sem=c_sem.at[1, i],
            device_id=(to * CORES + core, mt),
            device_id_type=MESH,
        )

    def value_arrival(i):
        to, source = other(i)
        return pltpu.make_async_remote_copy(
            src_ref=rows_of(csend, to),
            dst_ref=rows_of(crecv, source),
            send_sem=c_sem.at[0, i],
            recv_sem=c_sem.at[1, i],
            device_id=(to * CORES + core, mt),
            device_id_type=MESH,
        )

    each(0, chips - 1, lambda i: value_copy(i).start())
    crecv[own_rows, :] = csend[own_rows, :]

    for copy in o_copies:
        copy.wait_recv()
    do_ref[...] = sum(dbuf_out[s].astype(F32) for s in range(m)).astype(BF16)
    stat_row = lax.broadcasted_iota(jnp.int32, (128, 128), 0)
    summing = pick((stat_row >= half_lanes) & (stat_row < half_lanes + 3))

    each(0, chips - 1, lambda i: value_arrival(i).wait_recv())
    arrived = crecv[...]
    levels = dot(arrived, summing).reshape(chips, block, 128)
    arrived = arrived.astype(F32).reshape(chips, block, 128)
    top = jnp.max(levels, axis=0, keepdims=True)
    share = jnp.exp2(levels - top)
    value = jnp.sum(arrived * share, axis=0) / jnp.sum(share, axis=0)
    low = lax.broadcasted_iota(jnp.int32, (p, 128), 1) < half_lanes
    values = []
    for h in range(0, heads, 2):
        right = pltpu.roll(value[(h + 1) * p : (h + 2) * p], half_lanes, 1)
        values.append(jnp.where(low, value[h * p : (h + 1) * p], right))
    values = jnp.concatenate(values, axis=1).astype(BF16)
    p_copies = []
    for c in range(chunks):
        obuf = outs[c]
        obuf[mt] = dot(values, op[:, c * chunk : (c + 1) * chunk]).astype(BF16)
        for dt in range(1, m):
            copy = row_copy(obuf, o_sem.at[c], dt)
            copy.start()
            p_copies.append(copy)
    for c in range(chunks):
        for copy in p_copies[c * (m - 1) : (c + 1) * (m - 1)]:
            copy.wait_recv()
        out = sum(outs[c][s].astype(F32) for s in range(m))
        po_ref[:, c * chunk : (c + 1) * chunk] = out.astype(BF16)
    each(0, chips - 1, lambda i: query_copy(i).wait_send())
    each(0, chips - 1, lambda i: value_copy(i).wait_send())
    for copy in l_copies + [cache_copy, rows_copy] + o_copies + p_copies:
        copy.wait_send()


def put_out(*refs):
    count = len(refs) // 2
    sem = refs[-1]
    copies = [
        pltpu.make_async_copy(refs[i], refs[count + i], sem.at[i]) for i in range(count)
    ]
    for copy in copies:
        copy.start()
    for copy in copies:
        copy.wait()


def local(n, m, *args):
    (pt, dt, pfill, dfill, pc, dc, ig, qg, lg, qd, ld, rd, qu, ru, ku, vu, op) = args
    p, width = pt.shape
    dd = dt.shape[0]
    own = -(-(p + dd) // 8) * 8
    extra = 16
    heads, nd, kl = ku.shape
    block = heads * p
    chips = n // CORES
    chunks = 2
    any_spec = pl.BlockSpec(memory_space=pltpu.HBM)
    vmem = pl.BlockSpec(memory_space=pltpu.VMEM)
    ig, lg = ig[None], lg[None]
    pc, qd, rd = pc.T, qd.T, rd.T
    dc, vu = jnp.swapaxes(dc, 1, 2), jnp.swapaxes(vu, 1, 2)
    cache = pc.shape[1]
    like = lambda a: pltpu.VMEM(a.shape, a.dtype)
    scratch = [
        *[like(a) for a in (pt, dt)],
        *[pltpu.SMEM(a.shape, a.dtype) for a in (pfill, dfill)],
        pltpu.VMEM((2, *pc.shape), BF16),
        *[like(a) for a in (dc, ig, qg, lg)],
        *[like(a) for a in (qd, ld, rd, qu, ru, ku, vu, op)],
        pltpu.VMEM((extra, width), F32),
        pltpu.VMEM((m, own, ld.shape[1] + qd.shape[0]), BF16),
        pltpu.VMEM((chips * block, 128), BF16),
        pltpu.VMEM((2, extra, pc.shape[0]), BF16),
        pltpu.VMEM((heads * nd + 128, 2 * cache), BF16),
        pltpu.VMEM((heads * nd, 2 * cache), BF16),
        pltpu.VMEM((chips * block, 128), BF16),
        pltpu.VMEM((chips * block, 128), BF16),
        pltpu.VMEM((m, dd, width), BF16),
        [pltpu.VMEM((m, p, width // chunks), BF16)] * chunks,
        pltpu.SemaphoreType.REGULAR,
        pltpu.SemaphoreType.DMA((17,)),
        pltpu.SemaphoreType.DMA((2, chips)),
        pltpu.SemaphoreType.DMA((2, m)),
        pltpu.SemaphoreType.DMA((2, chips)),
        pltpu.SemaphoreType.DMA((2, 2)),
        pltpu.SemaphoreType.DMA((2, m)),
        pltpu.SemaphoreType.DMA((chunks, 2, m)),
    ]
    held = pl.pallas_call(
        functools.partial(kernel, n, m),
        out_shape=(
            pltpu.VMEM((p, width), BF16),
            pltpu.VMEM((dd, width), BF16),
            pltpu.VMEM((p, pc.shape[0]), BF16),
            pltpu.VMEM((dd, pc.shape[0]), BF16),
        ),
        in_specs=[any_spec] * 17,
        out_specs=(vmem,) * 4,
        scratch_shapes=scratch,
        compiler_params=pltpu.CompilerParams(
            collective_id=0, has_side_effects=True, vmem_limit_bytes=60 * 1024 * 1024
        ),
    )(pt, dt, pfill, dfill, pc, dc, ig, qg, lg, qd, ld, rd, qu, ru, ku, vu, op)
    return pl.pallas_call(
        put_out,
        out_shape=tuple(jax.ShapeDtypeStruct(a.shape, a.dtype) for a in held),
        in_specs=[vmem] * len(held),
        out_specs=(any_spec,) * len(held),
        scratch_shapes=[pltpu.SemaphoreType.DMA((len(held),))],
        compiler_params=pltpu.CompilerParams(vmem_limit_bytes=1024 * 1024),
    )(*held)


def solution(mesh):
    placed = (
        P("kv", None),
        P("kv", None),
        P(),
        P("kv"),
        P("kv", None),
        P("kv", None, None),
        P(),
        P(),
        P(),
        P(None, "tp"),
        P(None, "tp"),
        P(),
        P(None, "tp"),
        P(None, "tp"),
        P("tp", None, None),
        P("tp", None, None),
        P("tp", None),
    )
    return jax.shard_map(
        functools.partial(local, mesh.shape["kv"], mesh.shape["tp"]),
        mesh=mesh,
        in_specs=placed,
        out_specs=(P("kv", None), P("kv", None), P("kv", None), P("kv", None)),
        check_vma=False,
    )
```
